32 devices in a mesh: sp: 4 (over z), tp: 4 (over y, x), dp: 2 (over core).
Axes of the slice: x: 2, y: 2, z: 4, core: 2. Of those that a mesh axis runs over, the one named last changes fastest.
Arguments:
- latents: bfloat16 [2, 1024, 4096], P('dp', ('sp', 'tp')), may hold values from -8 to 8
- cond: bfloat16 [2, 4096], P('dp', 'sp'), may hold values from -6 to 6
- cond_ctx: bfloat16 [4096], P('sp'), may hold values from -6 to 6
- context: bfloat16 [2, 1024, 4096], P('dp', 'sp'), may hold values from -8 to 8
- w_shift: bfloat16 [4096, 4096], P('sp', 'tp'), may hold values from -0.09375 to 0.09375
- w_scale: bfloat16 [4096, 4096], P('sp', 'tp'), may hold values from -0.09375 to 0.09375
- w_gate: bfloat16 [4096, 4096], P('sp', 'tp'), may hold values from -0.1875 to 0.1875
- gain_pre: bfloat16 [4096], replicated, may hold values from 0.099609375 to 1.8984375
- gain_post: bfloat16 [4096], replicated, may hold values from 0.099609375 to 1.8984375
- w_query: bfloat16 [4096, 1024], P('dp', 'tp'), may hold values from -0.09375 to 0.09375
- w_key: bfloat16 [4096, 1024], P('dp', 'tp'), may hold values from -0.09375 to 0.09375
- w_value: bfloat16 [4096, 2048], P('dp', 'tp'), may hold values from -0.09375 to 0.09375
- w_outgate: bfloat16 [4096, 2048], P('dp', 'tp'), may hold values from -0.09375 to 0.09375
- w_down: bfloat16 [4096, 32], replicated, may hold values from -0.25 to 0.25
- decay_up: bfloat16 [2, 16, 1024], P(None, None, 'tp'), may hold values from -1.5 to 1.5
- decay_bias: float32 [2, 1024], P(None, 'tp'), may hold values from -0.5 to 11
- head_gain: bfloat16 [2048], P('tp'), may hold values from 0.099609375 to 1.8984375
- w_out: bfloat16 [2048, 4096], P('tp', 'dp'), may hold values from -0.125 to 0.125
Outputs:
- mixer_out: bfloat16 [2, 1024, 4096], P('dp', ('sp', 'tp'))
The draws below stay inside these ranges and needn't reach their ends.
All inputs are finite; a program needn't handle non-finite values.
Results may differ from the reference program's by a relative error of at most 0.015.
Values may be sent and summed in bfloat16 or wider, within the bound.
A program may use at most 128 MiB of HBM per device.

```python
import jax
import jax.numpy as jnp
from jax import lax

D = 4096
HEADS = 4
DK_HEAD = 256
DV_HEAD = 512
RANK = 16
BLOCK = 128
CTX = 1024
TOK_DEV = 256
SAMPLES = 2
TOKENS = 1024
DK = 1024
DVAL = 2048
N_TP = 4


def draw_latents(key, part):
    key_noise, key_offset = jax.random.split(key, 2)
    noise_field = jax.random.normal(key_noise, (SAMPLES, TOKENS, D), jnp.float32)
    offsets = 0.25 * jax.random.normal(key_offset, (SAMPLES, TOKENS // TOK_DEV, 1, D), jnp.float32)
    shifted = noise_field.reshape(SAMPLES, TOKENS // TOK_DEV, TOK_DEV, D) + offsets
    return jnp.clip(shifted.reshape(SAMPLES, TOKENS, D), -8.0, 8.0).astype(jnp.bfloat16)


def draw_context(key, part):
    key_noise = jax.random.fold_in(jax.random.fold_in(key, 7), 0)
    noise_field = jax.random.normal(key_noise, (SAMPLES, CTX, D), jnp.float32)
    return jnp.clip(noise_field, -8.0, 8.0).astype(jnp.bfloat16)


def draw_decay_bias(key, part):
    key_pick, key_fast, key_middle, key_slow = jax.random.split(jax.random.fold_in(key, 11), 4)
    picks = jax.random.randint(key_pick, (2, DK), 0, 10)
    fast_values = jax.random.uniform(key_fast, (2, DK), jnp.float32, -0.5, 1.5)
    fast_share = 3
    middle_share = 7
    middle_values = jax.random.uniform(key_middle, (2, DK), jnp.float32, 7.5, 9.5)
    slow_values = jax.random.uniform(key_slow, (2, DK), jnp.float32, 9.5, 11.0)
    chosen = jnp.where(picks < fast_share, fast_values, jnp.where(picks < middle_share, middle_values, slow_values))
    return chosen.astype(jnp.float32)


def shard_levels(own_key, extent, pieces, smallest, top_value):
    loudness = 1.0
    for position, blocks in pieces:
        draws = jax.random.uniform(jax.random.fold_in(jax.random.fold_in(own_key, 6), position), (blocks,), jnp.float32, smallest / len(pieces), top_value / len(pieces))
        loudness = loudness * jnp.repeat(jnp.exp(draws), extent[position] // blocks).reshape((-1,) + (1,) * (len(extent) - 1 - position))
    return loudness


def scatter_about(rng, extent, scale, most, cuts=(), held_as=jnp.bfloat16):
    values = scale * jax.random.normal(rng, extent, jnp.float32)
    if cuts:
        values = values * shard_levels(rng, extent, cuts, -0.22, 0.18)
    return jnp.clip(values, -most, most).astype(held_as)


def setup_inputs(seed: int = 0) -> dict:
    arg_keys = jax.random.split(jax.random.key(seed), 19)
    latents = draw_latents(jax.random.fold_in(arg_keys[18], 71), 0)
    cond = scatter_about(arg_keys[1], (SAMPLES, D), 1.0, 6.0, ((0, 2), (1, 4)))
    cond_ctx = scatter_about(arg_keys[2], (D,), 1.0, 6.0, ((0, 4),))
    context = draw_context(jax.random.fold_in(arg_keys[18], 71), 0)
    w_shift = scatter_about(arg_keys[4], (D, D), D ** -0.5, 0.09375, ((0, 4), (1, 4)))
    w_scale = scatter_about(arg_keys[5], (D, D), D ** -0.5, 0.09375, ((0, 4), (1, 4)))
    w_gate = scatter_about(arg_keys[6], (D, D), (D // 4) ** -0.5, 0.1875, ((0, 4), (1, 4)))
    gain_pre = jnp.clip(1.0 + 0.18 * jax.random.normal(arg_keys[7], (D,), jnp.float32), 0.099609375, 1.8984375).astype(jnp.bfloat16)
    gain_post = jnp.clip(1.0 + 0.18 * jax.random.normal(arg_keys[8], (D,), jnp.float32), 0.099609375, 1.8984375).astype(jnp.bfloat16)
    w_query = scatter_about(arg_keys[9], (D, DK), D ** -0.5, 0.09375, ((0, 2), (1, 4)))
    w_key = scatter_about(arg_keys[10], (D, DK), D ** -0.5, 0.09375, ((0, 2), (1, 4)))
    w_value = scatter_about(arg_keys[11], (D, DVAL), D ** -0.5, 0.09375, ((0, 2), (1, 4)))
    w_outgate = scatter_about(arg_keys[12], (D, DVAL), D ** -0.5, 0.09375, ((0, 2), (1, 4)))
    w_down = scatter_about(arg_keys[13], (D, 2 * RANK), (D // 9) ** -0.5, 0.25)
    decay_up = scatter_about(arg_keys[14], (2, RANK, DK), RANK ** -0.5, 1.5, ((2, 4),))
    decay_bias = draw_decay_bias(jax.random.fold_in(arg_keys[18], 71), 0)
    head_gain = jnp.clip(1.0 + 0.18 * jax.random.normal(arg_keys[16], (DVAL,), jnp.float32), 0.099609375, 1.8984375).astype(jnp.bfloat16)
    w_out = scatter_about(arg_keys[17], (DVAL, D), DVAL ** -0.5, 0.125, ((0, 4), (1, 2)))
    return dict(latents=latents, cond=cond, cond_ctx=cond_ctx, context=context, w_shift=w_shift, w_scale=w_scale, w_gate=w_gate, gain_pre=gain_pre, gain_post=gain_post, w_query=w_query, w_key=w_key, w_value=w_value, w_outgate=w_outgate, w_down=w_down, decay_up=decay_up, decay_bias=decay_bias, head_gain=head_gain, w_out=w_out)


EPS = 1e-06
TAU = 16.0
HIGH_ACCURACY = lax.Precision.HIGHEST

def matmul(left, right):
    return jnp.dot(left, right, preferred_element_type=jnp.float32)

def rms_scale(vectors, gain):
    return vectors * lax.rsqrt(lax.optimization_barrier(jnp.mean(vectors * vectors, axis=-1, keepdims=True)) + EPS) * gain

def log_decays(lowrank, decay_up, decay_bias):
    result = []
    for direction in range(2):
        preact = matmul(lowrank[:, direction * RANK:(direction + 1) * RANK], decay_up[direction]) + decay_bias[direction]
        result.append(jax.nn.log_sigmoid(preact) / TAU)
    return result

def context_states(ctx_keys, ctx_values, forward_decay, backward_decay):
    keys_float = ctx_keys.astype(jnp.float32)
    values_float = ctx_values.astype(jnp.float32)
    running_decay_sum = jnp.cumsum(forward_decay, axis=0)
    weight_fwd = jnp.exp(running_decay_sum[-1:] - running_decay_sum)
    weight_bwd = jnp.exp(jnp.cumsum(backward_decay, axis=0) - backward_decay)
    start_fwd = jnp.dot((keys_float * weight_fwd).T, values_float, precision=HIGH_ACCURACY)
    start_bwd = jnp.dot((keys_float * weight_bwd).T, values_float, precision=HIGH_ACCURACY)
    return (start_fwd, start_bwd)

def recurrence(queries, keys_in, values, decays, start):
    count = queries.shape[0] // BLOCK

    def blocks(array):
        return array.reshape(count, BLOCK, array.shape[-1])
    causal = jnp.tril(jnp.ones((BLOCK, BLOCK), bool))[:, :, None]

    def advance(carried_state, inputs):
        query_block_tile, key_block_tile, value_block_tile, block_g = inputs
        running_decay_sum = jnp.cumsum(block_g, axis=0)
        decay_pairs = jnp.exp(jnp.where(causal, running_decay_sum[:, None, :] - running_decay_sum[None, :, :], -jnp.inf))
        scores = jnp.einsum('tk,tsk,sk->ts', query_block_tile, decay_pairs, key_block_tile, precision=HIGH_ACCURACY)
        output = jnp.dot(scores, value_block_tile, precision=HIGH_ACCURACY) + jnp.dot(query_block_tile * jnp.exp(running_decay_sum), carried_state, precision=HIGH_ACCURACY)
        final_state_value = running_decay_sum[-1]
        carried_state = carried_state * jnp.exp(final_state_value)[:, None] + jnp.dot((key_block_tile * jnp.exp(final_state_value - running_decay_sum)).T, value_block_tile, precision=HIGH_ACCURACY)
        return (carried_state, output)
    carried_state, output = lax.scan(advance, start, (blocks(queries), blocks(keys_in), blocks(values), blocks(decays)))
    return output.reshape(-1, values.shape[-1])

def reference(latents, cond, cond_ctx, context, w_shift, w_scale, w_gate, gain_pre, gain_post, w_query, w_key, w_value, w_outgate, w_down, decay_up, decay_bias, head_gain, w_out):
    activated = jax.nn.silu(cond.astype(jnp.float32)).astype(jnp.bfloat16)
    activated_ctx = jax.nn.silu(cond_ctx.astype(jnp.float32)).astype(jnp.bfloat16)[None, :]
    shift_vec = matmul(activated, w_shift)
    scale_vec = matmul(activated, w_scale)
    gate_vec = matmul(activated, w_gate)
    shift_ctx = matmul(activated_ctx, w_shift)[0]
    scale_ctx = matmul(activated_ctx, w_scale)[0]
    gain_in = gain_pre.astype(jnp.float32)
    gain_out = gain_post.astype(jnp.float32)
    gains_head = head_gain.astype(jnp.float32)
    heads_dev = HEADS // N_TP
    group_width = heads_dev * DV_HEAD
    outputs = []
    for sample in range(SAMPLES):
        latent_rows = latents[sample].astype(jnp.float32)
        modulated = (rms_scale(latent_rows, gain_in) * (1.0 + scale_vec[sample]) + shift_vec[sample]).astype(jnp.bfloat16)
        ctx_rows = context[sample].astype(jnp.float32)
        modulated_ctx = (rms_scale(ctx_rows, gain_in) * (1.0 + scale_ctx) + shift_ctx).astype(jnp.bfloat16)
        queries = matmul(modulated, w_query).astype(jnp.bfloat16)
        latent_keys = matmul(modulated, w_key).astype(jnp.bfloat16)
        values = matmul(modulated, w_value).astype(jnp.bfloat16)
        out_gate = matmul(modulated, w_outgate).astype(jnp.bfloat16)
        lowrank = matmul(modulated, w_down).astype(jnp.bfloat16)
        ctx_keys = matmul(modulated_ctx, w_key).astype(jnp.bfloat16)
        ctx_values = matmul(modulated_ctx, w_value).astype(jnp.bfloat16)
        ctx_lowrank = matmul(modulated_ctx, w_down).astype(jnp.bfloat16)
        decay_fwd, decay_bwd = log_decays(lowrank, decay_up, decay_bias)
        ctx_fwd, ctx_bwd = log_decays(ctx_lowrank, decay_up, decay_bias)
        head_rows = []
        for head_index in range(HEADS):
            key_lo = head_index * DK_HEAD
            value_lo = head_index * DV_HEAD
            start_fwd, start_bwd = context_states(ctx_keys[:, key_lo:key_lo + DK_HEAD], ctx_values[:, value_lo:value_lo + DV_HEAD], ctx_fwd[:, key_lo:key_lo + DK_HEAD], ctx_bwd[:, key_lo:key_lo + DK_HEAD])
            head_query_rows = queries[:, key_lo:key_lo + DK_HEAD].astype(jnp.float32) * DK_HEAD ** (-0.5)
            head_k = latent_keys[:, key_lo:key_lo + DK_HEAD].astype(jnp.float32)
            head_v = values[:, value_lo:value_lo + DV_HEAD].astype(jnp.float32)
            forward_out = recurrence(head_query_rows, head_k, head_v, decay_fwd[:, key_lo:key_lo + DK_HEAD], start_fwd)
            backward_out = jnp.flip(recurrence(jnp.flip(head_query_rows, 0), jnp.flip(head_k, 0), jnp.flip(head_v, 0), jnp.flip(decay_bwd[:, key_lo:key_lo + DK_HEAD], 0), start_bwd), 0)
            mixed_sum = forward_out + backward_out
            gated_rows = rms_scale(mixed_sum, gains_head[value_lo:value_lo + DV_HEAD]) * jax.nn.silu(out_gate[:, value_lo:value_lo + DV_HEAD].astype(jnp.float32))
            head_rows.append(gated_rows.astype(jnp.bfloat16))
        heads_out = jnp.concatenate(head_rows, axis=1)
        projected = jnp.zeros((TOKENS, D), jnp.float32)
        for group_index in range(N_TP):
            lower = group_index * group_width
            partial_value = matmul(heads_out[:, lower:lower + group_width], w_out[lower:lower + group_width]).astype(jnp.bfloat16)
            partial_value = lax.optimization_barrier(partial_value)
            projected = projected + partial_value.astype(jnp.float32)
        result_rows = latent_rows + gate_vec[sample] * rms_scale(projected, gain_out)
        outputs.append(result_rows.astype(jnp.bfloat16))
    return jnp.stack(outputs)
```

```python
import functools

import jax
import jax.numpy as jnp
from jax import lax
from jax.experimental import pallas as pl
from jax.experimental.pallas import tpu as pltpu
from jax.sharding import PartitionSpec as P

RANK = 16
EPS = 1e-06
TAU = 16.0
SUB = 64
CH = 4
MESH = pl.DeviceIdType.MESH
F32 = jnp.float32
BF16 = jnp.bfloat16


def dot(a, b, dims=((1,), (0,))):
    return lax.dot_general(a, b, (dims, ((), ())), preferred_element_type=F32)


def silu(v):
    return v / (1.0 + jnp.exp(-v))


def log_sigmoid(v):
    return jnp.minimum(v, 0.0) - jnp.log1p(jnp.exp(-jnp.abs(v)))


def tri_sum(tri, g):
    high = g.astype(BF16)
    low = (g - high.astype(F32)).astype(BF16)
    return dot(tri, high) + dot(tri, low)


def triangle(n, upper):
    row = lax.broadcasted_iota(jnp.int32, (n, n), 0)
    col = lax.broadcasted_iota(jnp.int32, (n, n), 1)
    keep = (col >= row) if upper else (col <= row)
    return jnp.where(keep, 1.0, 0.0).astype(BF16)


def kernel(
    n_sp, n_tp, n_dp,
    lat_ref, cond_ref, cctx_ref, ctx_ref, wsh_hbm, wsc_hbm, wga_hbm, gpre_ref, gpost_ref,
    wq_hbm, wk_hbm, wv_hbm, wg_hbm, wdown_ref, up_ref, bias_ref, hgain_ref, wout_hbm,
    out_ref,
    wsh, wsc, wga, wq, wk, wv, wg, wout,
    lat_all, rows_lat, rows_ctx, part, mod_sp, mod_full,
    qb, kb, vb, gb, cum_f, cum_b, intra, heads,
    kc, vc, st_a, st_b,
    ry, rz, rf, rb, sy, sz, sf, sb, ra_f, ra_b, sa_f, sa_b,
    rs_send, rs_recv,
    lc_sem, wsend, wrecv, lsend, lrecv, m1send, m1recv, m2send, m2recv,
    csend, crecv, asend, arecv, osend, orecv, own_sem,
):
    sp, tp, dp = lax.axis_index("sp"), lax.axis_index("tp"), lax.axis_index("dp")
    half = n_tp // 2
    ty, tx = tp // 2, tp % 2

    def to(k):
        return ((ty + k // 2) % half) * 2 + (tx + k % 2) % 2

    def source(k):
        return ((ty + half - k // 2) % half) * 2 + (tx + k % 2) % 2

    rows_own = lat_ref.shape[0]
    rows = rows_own * n_tp
    cb = part.shape[1]

    def remote(src, dst, s, r, dev):
        return pltpu.make_async_remote_copy(
            src_ref=src, dst_ref=dst, send_sem=s, recv_sem=r, device_id=dev, device_id_type=MESH
        )

    mod_copies = []
    for i, (a, b) in enumerate(((wsh_hbm, wsh), (wsc_hbm, wsc), (wga_hbm, wga))):
        c = pltpu.make_async_copy(a, b, lc_sem.at[i])
        c.start()
        mod_copies.append(c)
    own = pltpu.make_async_copy(lat_ref, lat_all.at[tp], own_sem.at[0])
    own.start()

    barrier = pltpu.get_barrier_semaphore()
    for k in range(1, n_tp):
        pl.semaphore_signal(barrier, inc=1, device_id={"tp": to(k)}, device_id_type=MESH)
    for k in range(1, n_sp):
        pl.semaphore_signal(
            barrier, inc=1, device_id={"sp": (sp + k) % n_sp}, device_id_type=MESH
        )
    for k in range(1, n_dp):
        pl.semaphore_signal(
            barrier, inc=1, device_id={"dp": (dp + k) % n_dp}, device_id_type=MESH
        )
    pl.semaphore_wait(barrier, n_tp + n_sp + n_dp - 3)

    hr = rows_own // 2
    lat_copies = {}

    def send_lat(k, h):
        c = remote(
            lat_ref.at[pl.ds(h * hr, hr)], lat_all.at[tp, pl.ds(h * hr, hr)],
            lsend.at[k - 1, h], lrecv.at[k - 1, h], {"tp": to(k)},
        )
        c.start()
        lat_copies[k, h] = c

    for k in range(1, n_tp - 1):
        send_lat(k, 0)

    weight_pairs = ((wk_hbm, wk), (wv_hbm, wv), (wq_hbm, wq), (wg_hbm, wg), (wout_hbm, wout))
    w_copies = []
    for i, (a, b) in enumerate(weight_pairs):
        c = pltpu.make_async_copy(a, b.at[dp], lc_sem.at[3 + i])
        c.start()
        group = [c]
        for k in range(1, n_dp):
            c = remote(a, b.at[dp], wsend.at[k - 1, i], wrecv.at[k - 1, i],
                       {"dp": (dp + k) % n_dp})
            c.start()
            group.append(c)
        w_copies.append(group)

    def weights_ready(i):
        w_copies[i][0].wait()
        for c in w_copies[i][1:]:
            c.wait_recv()

    shape = (16, cond_ref.shape[1])
    first = lax.broadcasted_iota(jnp.int32, shape, 0) == 0
    act = jnp.where(
        first,
        jnp.broadcast_to(silu(cond_ref[...].astype(F32)), shape),
        jnp.broadcast_to(silu(cctx_ref[...].astype(F32)), shape),
    ).astype(BF16)
    for c in mod_copies:
        c.wait()
    d_sh, d_sc, d_ga = dot(act, wsh[...]), dot(act, wsc[...]), dot(act, wga[...])
    part[...] = jnp.zeros_like(part)
    part[0:1] = d_sh[0:1]
    part[1:2] = d_sc[0:1]
    part[2:3] = d_ga[0:1]
    part[3:4] = d_sh[1:2]
    part[4:5] = d_sc[1:2]
    m1 = []
    for k in range(1, n_sp):
        c = remote(part, mod_sp.at[k - 1], m1send.at[k - 1], m1recv.at[k - 1],
                   {"sp": (sp + k) % n_sp})
        c.start()
        m1.append(c)
    total = part[...]
    for k, c in enumerate(m1):
        c.wait_recv()
        total = total + mod_sp[k]
    mod_full[tp] = total
    m2 = []
    for k in range(1, n_tp):
        c = remote(mod_full.at[tp], mod_full.at[tp], m2send.at[k - 1], m2recv.at[k - 1],
                   {"tp": to(k)})
        c.start()
        m2.append(c)
    for k in (n_tp - 1,):
        send_lat(k, 0)
        send_lat(k, 1)
    for k in range(1, n_tp - 1):
        send_lat(k, 1)
    for c in m2:
        c.wait_recv()

    def modulate(load, store, count, at):
        def step(r, carry):
            x = load(r * 16).astype(F32)
            inv = lax.rsqrt(jnp.mean(x * x, axis=-1, keepdims=True) + EPS)
            pieces = []
            for c in range(n_tp):
                gain = gpre_ref[:, c * cb : (c + 1) * cb].astype(F32)
                y = x[:, c * cb : (c + 1) * cb] * inv * gain
                y = y * (1.0 + mod_full[c, at + 1 : at + 2]) + mod_full[c, at : at + 1]
                pieces.append(y.astype(BF16))
            store(r * 16, jnp.concatenate(pieces, axis=1))
            return carry

        lax.fori_loop(0, count // 16, step, 0)

    def project(src, w):
        depth = w.shape[1]
        acc = dot(src[:, 0:depth], w[0])
        for d in range(1, n_dp):
            acc = acc + dot(src[:, d * depth : (d + 1) * depth], w[d])
        return acc.astype(BF16)

    def decays(src):
        low = dot(src[...], wdown_ref[...]).astype(BF16)
        return log_sigmoid(dot(low, up_ref[...]) + bias_ref[...]) * (1.0 / TAU)

    n_ctx = ctx_ref.shape[0]

    def store_ctx(r, val):
        rows_ctx[pl.ds(pl.multiple_of(r, 16), 16)] = val

    modulate(lambda r: ctx_ref[pl.ds(pl.multiple_of(r, 16), 16)], store_ctx, n_ctx, 3)
    weights_ready(0)
    weights_ready(1)
    dk = kb.shape[1]
    dv = vb.shape[1]
    kc[...] = project(rows_ctx, wk)
    vc[...] = project(rows_ctx, wv)
    g_ctx = decays(rows_ctx)
    cum = tri_sum(triangle(n_ctx, False), g_ctx)
    keys = kc[...].astype(F32)
    last = cum[n_ctx - 1 : n_ctx]
    key_f = (keys * jnp.exp(last[:, :dk] - cum[:, :dk])).astype(BF16)
    key_b = (keys * jnp.exp(cum[:, dk:] - g_ctx[:, dk:])).astype(BF16)
    st_a[...] = dot(vc[...], key_f, ((0,), (0,)))
    st_b[...] = dot(vc[...], key_b, ((0,), (0,)))
    tot_f = last[:, :dk]
    tot_b = last[:, dk:]

    up = {"sp": jnp.minimum(sp + 1, n_sp - 1)}
    down = {"sp": jnp.maximum(sp - 1, 0)}
    has_up = sp < n_sp - 1
    has_down = sp > 0
    cw = dv // CH

    def chunk(i):
        return pl.ds(i * cw, cw)

    def y_copy(i):
        return remote(sy.at[chunk(i)], ry.at[chunk(i)], csend.at[0, i], crecv.at[0, i], down)

    def z_copy(i):
        return remote(sz.at[chunk(i)], rz.at[chunk(i)], csend.at[1, i], crecv.at[1, i], up)

    def f_copy(i):
        return remote(sf.at[chunk(i)], rf.at[chunk(i)], csend.at[2, i], crecv.at[2, i], up)

    def b_copy(i):
        return remote(sb.at[chunk(i)], rb.at[chunk(i)], csend.at[3, i], crecv.at[3, i], down)

    a_f = remote(sa_f, ra_f, asend.at[0], arecv.at[0], down)
    a_b = remote(sa_b, ra_b, asend.at[1], arecv.at[1], up)

    @pl.when(jnp.logical_not(has_up))
    def _():
        ra_f[...] = jnp.zeros_like(ra_f)
        ry[...] = jnp.zeros_like(ry)

    @pl.when(jnp.logical_not(has_down))
    def _():
        ra_b[...] = jnp.zeros_like(ra_b)
        rz[...] = jnp.zeros_like(rz)

    @pl.when(has_up)
    def _():
        a_f.wait_recv()

    sa_f[...] = ra_f[...] + tot_f

    @pl.when(has_down)
    def _():
        a_f.start()
        a_b.wait_recv()

    sa_b[...] = ra_b[...] + tot_b

    @pl.when(has_up)
    def _():
        a_b.start()

    scale_f = jnp.exp(ra_f[0:1])
    scale_b = jnp.exp(ra_b[0:1])
    for i in range(CH):
        c = slice(i * cw, (i + 1) * cw)

        @pl.when(has_up)
        def _():
            y_copy(i).wait_recv()

        y = ry[c].astype(F32) + st_a[c] * scale_f
        sy[c] = y.astype(BF16)

        @pl.when(has_down)
        def _():
            y_copy(i).start()
            z_copy(i).wait_recv()

        z = rz[c].astype(F32) + st_b[c] * scale_b
        sz[c] = z.astype(BF16)

        @pl.when(has_up)
        def _():
            z_copy(i).start()

    @pl.when(jnp.logical_not(has_down))
    def _():
        rf[...] = sy[...]

    @pl.when(jnp.logical_not(has_up))
    def _():
        rb[...] = sz[...]

    def modulate_block(blk):
        def store(r, val):
            at = pl.multiple_of(blk * rows_own + r, 16)
            rows_lat[pl.ds(at, 16)] = val

        modulate(
            lambda r: lat_all[blk, pl.ds(pl.multiple_of(r, 16), 16)], store, rows_own, 0
        )

    own.wait()
    modulate_block(tp)
    for k in range(1, n_tp):
        lat_copies[k, 0].wait_recv()
        lat_copies[k, 1].wait_recv()
        modulate_block(source(k))

    kb[...] = project(rows_lat, wk)
    vb[...] = project(rows_lat, wv)
    g_lat = decays(rows_lat)
    cum_f[...] = tri_sum(triangle(rows, False), g_lat[:, :dk])
    cum_b[...] = tri_sum(triangle(rows, True), g_lat[:, dk:])
    keys = kb[...].astype(F32)
    end_f = cum_f[rows - 1 : rows]
    end_b = cum_b[0:1]
    key_f = (keys * jnp.exp(end_f - cum_f[...])).astype(BF16)
    key_b = (keys * jnp.exp(end_b - cum_b[...])).astype(BF16)
    st_a[...] = dot(vb[...], key_f, ((0,), (0,)))
    st_b[...] = dot(vb[...], key_b, ((0,), (0,)))
    step_f = jnp.exp(end_f)
    step_b = jnp.exp(end_b)

    def relay(i):
        c = slice(i * cw, (i + 1) * cw)

        @pl.when(has_down)
        def _():
            f_copy(i).wait_recv()

        sf[c] = (rf[c].astype(F32) * step_f + st_a[c]).astype(BF16)

        @pl.when(has_up)
        def _():
            f_copy(i).start()
            b_copy(i).wait_recv()

        sb[c] = (rb[c].astype(F32) * step_b + st_b[c]).astype(BF16)

        @pl.when(has_down)
        def _():
            b_copy(i).start()

    weights_ready(2)
    weights_ready(3)
    qb[...] = project(rows_lat, wq)
    gb[...] = project(rows_lat, wg)

    scale = dk ** -0.5
    n_sub = rows // SUB

    def block_scores(i):
        lo, hi, mid = i * SUB, (i + 1) * SUB, i * SUB + SUB // 2
        q = qb[lo:hi].astype(F32) * scale
        r_f = cum_f[mid : mid + 1]
        s_f = dot(
            (q * jnp.exp(cum_f[lo:hi] - r_f)).astype(BF16),
            (kb[0:hi].astype(F32) * jnp.exp(r_f - cum_f[0:hi])).astype(BF16),
            ((1,), (1,)),
        )
        t = lax.broadcasted_iota(jnp.int32, (SUB, hi), 0) + lo
        s = lax.broadcasted_iota(jnp.int32, (SUB, hi), 1)
        s_f = jnp.where(s <= t, s_f, 0.0)
        r_b = cum_b[mid : mid + 1]
        s_b = dot(
            (q * jnp.exp(cum_b[lo:hi] - r_b)).astype(BF16),
            (kb[lo:rows].astype(F32) * jnp.exp(r_b - cum_b[lo:rows])).astype(BF16),
            ((1,), (1,)),
        )
        t = lax.broadcasted_iota(jnp.int32, (SUB, rows - lo), 0)
        s = lax.broadcasted_iota(jnp.int32, (SUB, rows - lo), 1)
        s_b = jnp.where(s >= t, s_b, 0.0)
        intra[lo:hi] = dot(s_f.astype(BF16), vb[0:hi]) + dot(s_b.astype(BF16), vb[lo:rows])

    for i in range(CH):
        relay(i)
    for i in range(n_sub):
        block_scores(i)

    q = qb[...].astype(F32) * scale
    q_f = (q * jnp.exp(cum_f[...])).astype(BF16)
    q_b = (q * jnp.exp(cum_b[...])).astype(BF16)
    mixed = intra[...] + dot(q_f, rf[...], ((1,), (1,))) + dot(q_b, rb[...], ((1,), (1,)))
    inv = lax.rsqrt(jnp.mean(mixed * mixed, axis=-1, keepdims=True) + EPS)
    gated = mixed * inv * hgain_ref[...].astype(F32) * silu(gb[...].astype(F32))
    heads[...] = gated.astype(BF16)

    weights_ready(4)
    out_copies = []
    wc = wout.shape[2]
    for k in list(range(n_tp - 1, 0, -1)) + [0]:
        h = heads[pl.ds(pl.multiple_of(to(k) * rows_own, rows_own), rows_own)]
        for d in range(n_dp):
            rs_send[k, d] = dot(h, wout[d]).astype(BF16)
            if k:
                c = remote(rs_send.at[k, d], rs_recv.at[k - 1, d], osend.at[k - 1, d],
                           orecv.at[k - 1, d], {"tp": to(k)})
                c.start()
                out_copies.append(c)
    for c in out_copies:
        c.wait_recv()

    def finish(r, carry):
        at = pl.ds(pl.multiple_of(r * 16, 16), 16)
        proj = []
        for d in range(n_dp):
            v = rs_send[0, d, at].astype(F32)
            for k in range(1, n_tp):
                v = v + rs_recv[k - 1, d, at].astype(F32)
            proj.append(v)
        v = jnp.concatenate(proj, axis=1)
        inv = lax.rsqrt(jnp.mean(v * v, axis=-1, keepdims=True) + EPS)
        x = lat_ref[at].astype(F32)
        for c in range(n_tp):
            cols = slice(c * cb, (c + 1) * cb)
            y = v[:, cols] * inv * gpost_ref[:, cols].astype(F32)
            out_ref[at, cols] = (x[:, cols] + mod_full[c, 2:3] * y).astype(BF16)
        return carry

    lax.fori_loop(0, rows_own // 16, finish, 0)

    for c in out_copies + m1 + m2 + list(lat_copies.values()):
        c.wait_send()
    for group in w_copies:
        for c in group[1:]:
            c.wait_send()

    @pl.when(has_down)
    def _():
        a_f.wait_send()
        for i in range(CH):
            y_copy(i).wait_send()
            b_copy(i).wait_send()

    @pl.when(has_up)
    def _():
        a_b.wait_send()
        for i in range(CH):
            z_copy(i).wait_send()
            f_copy(i).wait_send()


def body(
    latents, cond, cond_ctx, context, w_shift, w_scale, w_gate, gain_pre, gain_post,
    w_query, w_key, w_value, w_outgate, w_down, decay_up, decay_bias, head_gain, w_out,
):
    n_sp, n_tp, n_dp = lax.axis_size("sp"), lax.axis_size("tp"), lax.axis_size("dp")
    width = gain_pre.shape[0]
    rows_own = latents.shape[1]
    rows = rows_own * n_tp
    n_ctx = context.shape[1]
    dk, dv = w_key.shape[1], w_value.shape[1]
    depth = w_key.shape[0]
    zero = jnp.zeros_like(decay_up[0])
    up = jnp.concatenate(
        [
            jnp.concatenate([decay_up[0], zero], axis=1),
            jnp.concatenate([zero, decay_up[1]], axis=1),
        ],
        axis=0,
    )
    mod_in, mod_cols = w_shift.shape
    vm = pl.BlockSpec(memory_space=pltpu.VMEM)
    hbm = pl.BlockSpec(memory_space=pl.ANY)
    V, D = pltpu.VMEM, pltpu.SemaphoreType.DMA
    scratch = [
        V((mod_in, mod_cols), BF16), V((mod_in, mod_cols), BF16), V((mod_in, mod_cols), BF16),
        V((n_dp, depth, dk), BF16), V((n_dp, depth, dk), BF16),
        V((n_dp, depth, dv), BF16), V((n_dp, depth, dv), BF16),
        V((n_dp,) + w_out.shape, BF16),
        V((n_tp, rows_own, width), BF16), V((rows, width), BF16), V((n_ctx, width), BF16),
        V((8, mod_cols), F32), V((max(n_sp - 1, 1), 8, mod_cols), F32),
        V((n_tp, 8, mod_cols), F32),
        V((rows, dk), BF16), V((rows, dk), BF16), V((rows, dv), BF16), V((rows, dv), BF16),
        V((rows, dk), F32), V((rows, dk), F32), V((rows, dv), F32), V((rows, dv), BF16),
        V((n_ctx, dk), BF16), V((n_ctx, dv), BF16), V((dv, dk), F32), V((dv, dk), F32),
    ]
    scratch += [V((dv, dk), BF16)] * 8
    scratch += [V((8, dk), F32)] * 4
    scratch += [
        V((n_tp,  n_dp, rows_own, w_out.shape[1]), BF16),
        V((n_tp - 1, n_dp, rows_own, w_out.shape[1]), BF16),
        D((8,)), D((n_dp - 1, 5)), D((n_dp - 1, 5)), D((n_tp - 1, 2)), D((n_tp - 1, 2)),
        D((n_sp - 1,)), D((n_sp - 1,)), D((n_tp - 1,)), D((n_tp - 1,)),
        D((4, CH)), D((4, CH)), D((2,)), D((2,)),
        D((n_tp - 1, n_dp)), D((n_tp - 1, n_dp)), D((1,)),
    ]
    out = pl.pallas_call(
        functools.partial(kernel, n_sp, n_tp, n_dp),
        out_shape=jax.ShapeDtypeStruct((rows_own, width), BF16),
        in_specs=[vm, vm, vm, vm, hbm, hbm, hbm, vm, vm, hbm, hbm, hbm, hbm, vm, vm, vm, vm, hbm],
        out_specs=vm,
        scratch_shapes=scratch,
        compiler_params=pltpu.CompilerParams(
            collective_id=0, has_side_effects=True, vmem_limit_bytes=60 * 1024 * 1024
        ),
    )(
        latents[0], cond, cond_ctx[None], context[0], w_shift, w_scale, w_gate,
        gain_pre[None], gain_post[None], w_query, w_key, w_value, w_outgate, w_down, up,
        decay_bias.reshape(1, -1), head_gain[None], w_out,
    )
    return out[None]


def solution(mesh):
    return jax.shard_map(
        body,
        mesh=mesh,
        in_specs=(
            P("dp", ("sp", "tp"), None),
            P("dp", "sp"),
            P("sp"),
            P("dp", "sp", None),
            P("sp", "tp"),
            P("sp", "tp"),
            P("sp", "tp"),
            P(),
            P(),
            P("dp", "tp"),
            P("dp", "tp"),
            P("dp", "tp"),
            P("dp", "tp"),
            P(),
            P(None, None, "tp"),
            P(None, "tp"),
            P("tp"),
            P("tp", "dp"),
        ),
        out_specs=P("dp", ("sp", "tp"), None),
        check_vma=False,
    )
```

```python
import functools

import jax
import jax.numpy as jnp
from jax import lax
from jax.experimental import pallas as pl
from jax.experimental.pallas import tpu as pltpu
from jax.sharding import PartitionSpec as P

RANK = 16
EPS = 1e-06
TAU = 16.0
SUB = 64
CH = 4
MESH = pl.DeviceIdType.MESH
F32 = jnp.float32
BF16 = jnp.bfloat16


def dot(a, b, dims=((1,), (0,))):
    return lax.dot_general(a, b, (dims, ((), ())), preferred_element_type=F32)


def silu(v):
    return v / (1.0 + jnp.exp(-v))


def log_sigmoid(v):
    return jnp.minimum(v, 0.0) - jnp.log1p(jnp.exp(-jnp.abs(v)))


def tri_sum(tri, g):
    high = g.astype(BF16)
    low = (g - high.astype(F32)).astype(BF16)
    return dot(tri, high) + dot(tri, low)


def triangle(n, upper):
    row = lax.broadcasted_iota(jnp.int32, (n, n), 0)
    col = lax.broadcasted_iota(jnp.int32, (n, n), 1)
    keep = (col >= row) if upper else (col <= row)
    return jnp.where(keep, 1.0, 0.0).astype(BF16)


def kernel(
    n_sp, n_tp, n_dp,
    lat3, cond_ref, vec_ref, ctx3, wsh_hbm, wsc_hbm, wga_hbm,
    wq_hbm, wk_hbm, wv_hbm, wg_hbm, wdown_ref, up_ref, bias_ref, wout_hbm,
    out3,
    wsh, wsc, wga, wq, wk, wv, wg, wout,
    lat_all, rows_lat, rows_ctx, part, mod_sp, mod_full,
    qb, kb, vb, gb, cum_f, cum_b, intra, heads,
    kc, vc, st_a, st_b,
    ry, rz, rf, rb, sy, sz, sf, sb, ra_f, ra_b, sa_f, sa_b,
    rs_send, rs_recv,
    lc_sem, wsend, wrecv, lsend, lrecv, m1send, m1recv, m2send, m2recv,
    csend, crecv, asend, arecv, osend, orecv, own_sem,
):
    sp, tp, dp = lax.axis_index("sp"), lax.axis_index("tp"), lax.axis_index("dp")
    half = n_tp // 2
    ty, tx = tp // 2, tp % 2

    def to(k):
        return ((ty + k // 2) % half) * 2 + (tx + k % 2) % 2

    def source(k):
        return ((ty + half - k // 2) % half) * 2 + (tx + k % 2) % 2

    lat_ref, ctx_ref, out_ref = lat3.at[0], ctx3.at[0], out3.at[0]
    rows_own, width = lat_ref.shape
    n_cond, n_head = cond_ref.shape[1], vb.shape[1]
    gpre_ref = vec_ref.at[:, pl.ds(0, width)]
    gpost_ref = vec_ref.at[:, pl.ds(width, width)]
    cctx_ref = vec_ref.at[:, pl.ds(2 * width, n_cond)]
    hgain_ref = vec_ref.at[:, pl.ds(2 * width + n_cond, n_head)]
    rows = rows_own * n_tp
    cb = part.shape[1]

    def remote(src, dst, s, r, dev):
        return pltpu.make_async_remote_copy(
            src_ref=src, dst_ref=dst, send_sem=s, recv_sem=r, device_id=dev, device_id_type=MESH
        )

    mod_copies = []
    for i, (a, b) in enumerate(((wsh_hbm, wsh), (wsc_hbm, wsc), (wga_hbm, wga))):
        c = pltpu.make_async_copy(a, b, lc_sem.at[i])
        c.start()
        mod_copies.append(c)
    own = pltpu.make_async_copy(lat_ref, lat_all.at[tp], own_sem.at[0])
    own.start()

    barrier = pltpu.get_barrier_semaphore()
    for k in range(1, n_tp):
        pl.semaphore_signal(barrier, inc=1, device_id={"tp": to(k)}, device_id_type=MESH)
    for k in range(1, n_sp):
        pl.semaphore_signal(
            barrier, inc=1, device_id={"sp": (sp + k) % n_sp}, device_id_type=MESH
        )
    for k in range(1, n_dp):
        pl.semaphore_signal(
            barrier, inc=1, device_id={"dp": (dp + k) % n_dp}, device_id_type=MESH
        )
    pl.semaphore_wait(barrier, n_tp + n_sp + n_dp - 3)

    hr = rows_own // 2
    lat_copies = {}

    def send_lat(k, h):
        c = remote(
            lat_ref.at[pl.ds(h * hr, hr)], lat_all.at[tp, pl.ds(h * hr, hr)],
            lsend.at[k - 1, h], lrecv.at[k - 1, h], {"tp": to(k)},
        )
        c.start()
        lat_copies[k, h] = c

    for k in range(1, n_tp - 1):
        send_lat(k, 0)

    weight_pairs = ((wk_hbm, wk), (wv_hbm, wv), (wq_hbm, wq), (wg_hbm, wg), (wout_hbm, wout))
    w_copies = []
    for i, (a, b) in enumerate(weight_pairs):
        c = pltpu.make_async_copy(a, b.at[dp], lc_sem.at[3 + i])
        c.start()
        group = [c]
        for k in range(1, n_dp):
            c = remote(a, b.at[dp], wsend.at[k - 1, i], wrecv.at[k - 1, i],
                       {"dp": (dp + k) % n_dp})
            c.start()
            group.append(c)
        w_copies.append(group)

    def weights_ready(i):
        w_copies[i][0].wait()
        for c in w_copies[i][1:]:
            c.wait_recv()

    shape = (16, cond_ref.shape[1])
    first = lax.broadcasted_iota(jnp.int32, shape, 0) == 0
    act = jnp.where(
        first,
        jnp.broadcast_to(silu(cond_ref[...].astype(F32)), shape),
        jnp.broadcast_to(silu(cctx_ref[...].astype(F32)), shape),
    ).astype(BF16)
    for c in mod_copies:
        c.wait()
    d_sh, d_sc, d_ga = dot(act, wsh[...]), dot(act, wsc[...]), dot(act, wga[...])
    part[...] = jnp.zeros_like(part)
    part[0:1] = d_sh[0:1]
    part[1:2] = d_sc[0:1]
    part[2:3] = d_ga[0:1]
    part[3:4] = d_sh[1:2]
    part[4:5] = d_sc[1:2]
    m1 = []
    for k in range(1, n_sp):
        c = remote(part, mod_sp.at[k - 1], m1send.at[k - 1], m1recv.at[k - 1],
                   {"sp": (sp + k) % n_sp})
        c.start()
        m1.append(c)
    total = part[...]
    for k, c in enumerate(m1):
        c.wait_recv()
        total = total + mod_sp[k]
    mod_full[tp] = total
    m2 = []
    for k in range(1, n_tp):
        c = remote(mod_full.at[tp], mod_full.at[tp], m2send.at[k - 1], m2recv.at[k - 1],
                   {"tp": to(k)})
        c.start()
        m2.append(c)
    for k in (n_tp - 1,):
        send_lat(k, 0)
        send_lat(k, 1)
    for k in range(1, n_tp - 1):
        send_lat(k, 1)
    for c in m2:
        c.wait_recv()

    def modulate(load, store, count, at):
        def step(r, carry):
            x = load(r * 16).astype(F32)
            inv = lax.rsqrt(jnp.mean(x * x, axis=-1, keepdims=True) + EPS)
            pieces = []
            for c in range(n_tp):
                gain = gpre_ref[:, c * cb : (c + 1) * cb].astype(F32)
                y = x[:, c * cb : (c + 1) * cb] * inv * gain
                y = y * (1.0 + mod_full[c, at + 1 : at + 2]) + mod_full[c, at : at + 1]
                pieces.append(y.astype(BF16))
            store(r * 16, jnp.concatenate(pieces, axis=1))
            return carry

        lax.fori_loop(0, count // 16, step, 0)

    def project(src, w):
        depth = w.shape[1]
        acc = dot(src[:, 0:depth], w[0])
        for d in range(1, n_dp):
            acc = acc + dot(src[:, d * depth : (d + 1) * depth], w[d])
        return acc.astype(BF16)

    def decays(src):
        low = dot(src[...], wdown_ref[...], ((1,), (1,))).astype(BF16)
        zero = jnp.zeros_like(up_ref[0])
        both = jnp.concatenate(
            [
                jnp.concatenate([up_ref[0], zero], axis=1),
                jnp.concatenate([zero, up_ref[1]], axis=1),
            ],
            axis=0,
        )
        bias = jnp.concatenate([bias_ref[0:1], bias_ref[1:2]], axis=1)
        return log_sigmoid(dot(low, both) + bias) * (1.0 / TAU)

    n_ctx = ctx_ref.shape[0]

    def store_ctx(r, val):
        rows_ctx[pl.ds(pl.multiple_of(r, 16), 16)] = val

    modulate(lambda r: ctx_ref[pl.ds(pl.multiple_of(r, 16), 16)], store_ctx, n_ctx, 3)
    weights_ready(0)
    weights_ready(1)
    dk = kb.shape[1]
    dv = vb.shape[1]
    kc[...] = project(rows_ctx, wk)
    vc[...] = project(rows_ctx, wv)
    g_ctx = decays(rows_ctx)
    cum = tri_sum(triangle(n_ctx, False), g_ctx)
    keys = kc[...].astype(F32)
    last = cum[n_ctx - 1 : n_ctx]
    key_f = (keys * jnp.exp(last[:, :dk] - cum[:, :dk])).astype(BF16)
    key_b = (keys * jnp.exp(cum[:, dk:] - g_ctx[:, dk:])).astype(BF16)
    st_a[...] = dot(vc[...], key_f, ((0,), (0,)))
    st_b[...] = dot(vc[...], key_b, ((0,), (0,)))
    tot_f = last[:, :dk]
    tot_b = last[:, dk:]

    up = {"sp": jnp.minimum(sp + 1, n_sp - 1)}
    down = {"sp": jnp.maximum(sp - 1, 0)}
    has_up = sp < n_sp - 1
    has_down = sp > 0
    cw = dv // CH

    def chunk(i):
        return pl.ds(i * cw, cw)

    def y_copy(i):
        return remote(sy.at[chunk(i)], ry.at[chunk(i)], csend.at[0, i], crecv.at[0, i], down)

    def z_copy(i):
        return remote(sz.at[chunk(i)], rz.at[chunk(i)], csend.at[1, i], crecv.at[1, i], up)

    def f_copy(i):
        return remote(sf.at[chunk(i)], rf.at[chunk(i)], csend.at[2, i], crecv.at[2, i], up)

    def b_copy(i):
        return remote(sb.at[chunk(i)], rb.at[chunk(i)], csend.at[3, i], crecv.at[3, i], down)

    a_f = remote(sa_f, ra_f, asend.at[0], arecv.at[0], down)
    a_b = remote(sa_b, ra_b, asend.at[1], arecv.at[1], up)

    @pl.when(jnp.logical_not(has_up))
    def _():
        ra_f[...] = jnp.zeros_like(ra_f)
        ry[...] = jnp.zeros_like(ry)

    @pl.when(jnp.logical_not(has_down))
    def _():
        ra_b[...] = jnp.zeros_like(ra_b)
        rz[...] = jnp.zeros_like(rz)

    def a_down():
        @pl.when(has_up)
        def _():
            a_f.wait_recv()

        sa_f[...] = ra_f[...] + tot_f

        @pl.when(has_down)
        def _():
            a_f.start()

    def a_up():
        @pl.when(has_down)
        def _():
            a_b.wait_recv()

        sa_b[...] = ra_b[...] + tot_b

        @pl.when(has_up)
        def _():
            a_b.start()

    lower = 2 * sp < n_sp
    upper = jnp.logical_not(lower)
    pl.when(lower)(a_up)
    pl.when(upper)(a_down)
    pl.when(lower)(a_down)
    pl.when(upper)(a_up)

    scale_f = jnp.exp(ra_f[0:1])
    scale_b = jnp.exp(ra_b[0:1])
    def modulate_block(blk):
        def store(r, val):
            at = pl.multiple_of(blk * rows_own + r, 16)
            rows_lat[pl.ds(at, 16)] = val

        modulate(
            lambda r: lat_all[blk, pl.ds(pl.multiple_of(r, 16), 16)], store, rows_own, 0
        )

    def y_pass():
        for i in range(CH):
            c = slice(i * cw, (i + 1) * cw)

            @pl.when(has_up)
            def _():
                y_copy(i).wait_recv()

            sy[c] = (ry[c].astype(F32) + st_a[c] * scale_f).astype(BF16)

            @pl.when(has_down)
            def _():
                y_copy(i).start()

    def z_pass():
        for i in range(CH):
            c = slice(i * cw, (i + 1) * cw)

            @pl.when(has_down)
            def _():
                z_copy(i).wait_recv()

            sz[c] = (rz[c].astype(F32) + st_b[c] * scale_b).astype(BF16)

            @pl.when(has_up)
            def _():
                z_copy(i).start()

    pl.when(lower)(z_pass)
    pl.when(upper)(y_pass)
    own.wait()
    modulate_block(tp)
    pl.when(lower)(y_pass)
    pl.when(upper)(z_pass)

    @pl.when(jnp.logical_not(has_down))
    def _():
        rf[...] = sy[...]

    @pl.when(jnp.logical_not(has_up))
    def _():
        rb[...] = sz[...]

    for k in range(1, n_tp):
        lat_copies[k, 0].wait_recv()
        lat_copies[k, 1].wait_recv()
        modulate_block(source(k))

    kb[...] = project(rows_lat, wk)
    vb[...] = project(rows_lat, wv)
    g_lat = decays(rows_lat)
    cum_f[...] = tri_sum(triangle(rows, False), g_lat[:, :dk])
    cum_b[...] = tri_sum(triangle(rows, True), g_lat[:, dk:])
    keys = kb[...].astype(F32)
    end_f = cum_f[rows - 1 : rows]
    end_b = cum_b[0:1]
    key_f = (keys * jnp.exp(end_f - cum_f[...])).astype(BF16)
    key_b = (keys * jnp.exp(end_b - cum_b[...])).astype(BF16)
    st_a[...] = dot(vb[...], key_f, ((0,), (0,)))
    st_b[...] = dot(vb[...], key_b, ((0,), (0,)))
    step_f = jnp.exp(end_f)
    step_b = jnp.exp(end_b)

    def f_pass():
        for i in range(CH):
            c = slice(i * cw, (i + 1) * cw)

            @pl.when(has_down)
            def _():
                f_copy(i).wait_recv()

            @pl.when(has_up)
            def _():
                sf[c] = (rf[c].astype(F32) * step_f + st_a[c]).astype(BF16)
                f_copy(i).start()

    def b_pass():
        for i in range(CH):
            c = slice(i * cw, (i + 1) * cw)

            @pl.when(has_up)
            def _():
                b_copy(i).wait_recv()

            @pl.when(has_down)
            def _():
                sb[c] = (rb[c].astype(F32) * step_b + st_b[c]).astype(BF16)
                b_copy(i).start()

    pl.when(lower)(f_pass)
    pl.when(upper)(b_pass)

    weights_ready(2)
    weights_ready(3)
    qb[...] = project(rows_lat, wq)
    gb[...] = project(rows_lat, wg)

    scale = dk ** -0.5
    n_sub = rows // SUB

    def block_scores(i):
        lo, hi, mid = i * SUB, (i + 1) * SUB, i * SUB + SUB // 2
        q = qb[lo:hi].astype(F32) * scale
        r_f = cum_f[mid : mid + 1]
        s_f = dot(
            (q * jnp.exp(cum_f[lo:hi] - r_f)).astype(BF16),
            (kb[0:hi].astype(F32) * jnp.exp(r_f - cum_f[0:hi])).astype(BF16),
            ((1,), (1,)),
        )
        t = lax.broadcasted_iota(jnp.int32, (SUB, hi), 0) + lo
        s = lax.broadcasted_iota(jnp.int32, (SUB, hi), 1)
        s_f = jnp.where(s <= t, s_f, 0.0)
        r_b = cum_b[mid : mid + 1]
        s_b = dot(
            (q * jnp.exp(cum_b[lo:hi] - r_b)).astype(BF16),
            (kb[lo:rows].astype(F32) * jnp.exp(r_b - cum_b[lo:rows])).astype(BF16),
            ((1,), (1,)),
        )
        t = lax.broadcasted_iota(jnp.int32, (SUB, rows - lo), 0)
        s = lax.broadcasted_iota(jnp.int32, (SUB, rows - lo), 1)
        s_b = jnp.where(s >= t, s_b, 0.0)
        intra[lo:hi] = dot(s_f.astype(BF16), vb[0:hi]) + dot(s_b.astype(BF16), vb[lo:rows])

    for i in range(n_sub):
        block_scores(i)
    pl.when(lower)(b_pass)
    pl.when(upper)(f_pass)

    q = qb[...].astype(F32) * scale
    q_f = (q * jnp.exp(cum_f[...])).astype(BF16)
    q_b = (q * jnp.exp(cum_b[...])).astype(BF16)
    mixed = intra[...] + dot(q_f, rf[...], ((1,), (1,))) + dot(q_b, rb[...], ((1,), (1,)))
    inv = lax.rsqrt(jnp.mean(mixed * mixed, axis=-1, keepdims=True) + EPS)
    gated = mixed * inv * hgain_ref[...].astype(F32) * silu(gb[...].astype(F32))
    heads[...] = gated.astype(BF16)

    weights_ready(4)
    out_copies = []
    wc = wout.shape[2]
    for k in list(range(n_tp - 1, 0, -1)) + [0]:
        h = heads[pl.ds(pl.multiple_of(to(k) * rows_own, rows_own), rows_own)]
        for d in range(n_dp):
            rs_send[k, d] = dot(h, wout[d]).astype(BF16)
            if k:
                c = remote(rs_send.at[k, d], rs_recv.at[k - 1, d], osend.at[k - 1, d],
                           orecv.at[k - 1, d], {"tp": to(k)})
                c.start()
                out_copies.append(c)
    for c in out_copies:
        c.wait_recv()

    def finish(r, carry):
        at = pl.ds(pl.multiple_of(r * 16, 16), 16)
        proj = []
        for d in range(n_dp):
            v = rs_send[0, d, at].astype(F32)
            for k in range(1, n_tp):
                v = v + rs_recv[k - 1, d, at].astype(F32)
            proj.append(v)
        v = jnp.concatenate(proj, axis=1)
        inv = lax.rsqrt(jnp.mean(v * v, axis=-1, keepdims=True) + EPS)
        x = lat_ref[at].astype(F32)
        for c in range(n_tp):
            cols = slice(c * cb, (c + 1) * cb)
            y = v[:, cols] * inv * gpost_ref[:, cols].astype(F32)
            out_ref[at, cols] = (x[:, cols] + mod_full[c, 2:3] * y).astype(BF16)
        return carry

    lax.fori_loop(0, rows_own // 16, finish, 0)

    for c in out_copies + m1 + m2 + list(lat_copies.values()):
        c.wait_send()
    for group in w_copies:
        for c in group[1:]:
            c.wait_send()

    @pl.when(has_down)
    def _():
        a_f.wait_send()
        for i in range(CH):
            y_copy(i).wait_send()
            b_copy(i).wait_send()

    @pl.when(has_up)
    def _():
        a_b.wait_send()
        for i in range(CH):
            z_copy(i).wait_send()
            f_copy(i).wait_send()


def body(
    latents, cond, cond_ctx, context, w_shift, w_scale, w_gate, gain_pre, gain_post,
    w_query, w_key, w_value, w_outgate, w_down, decay_up, decay_bias, head_gain, w_out,
):
    n_sp, n_tp, n_dp = lax.axis_size("sp"), lax.axis_size("tp"), lax.axis_size("dp")
    width = gain_pre.shape[0]
    rows_own = latents.shape[1]
    rows = rows_own * n_tp
    n_ctx = context.shape[1]
    dk, dv = w_key.shape[1], w_value.shape[1]
    depth = w_key.shape[0]
    vectors = lax.optimization_barrier(
        jnp.concatenate([gain_pre, gain_post, cond_ctx, head_gain])
    )[None]
    mod_in, mod_cols = w_shift.shape
    vm = pl.BlockSpec(memory_space=pltpu.VMEM)
    hbm = pl.BlockSpec(memory_space=pl.ANY)
    V, D = pltpu.VMEM, pltpu.SemaphoreType.DMA
    scratch = [
        V((mod_in, mod_cols), BF16), V((mod_in, mod_cols), BF16), V((mod_in, mod_cols), BF16),
        V((n_dp, depth, dk), BF16), V((n_dp, depth, dk), BF16),
        V((n_dp, depth, dv), BF16), V((n_dp, depth, dv), BF16),
        V((n_dp,) + w_out.shape, BF16),
        V((n_tp, rows_own, width), BF16), V((rows, width), BF16), V((n_ctx, width), BF16),
        V((8, mod_cols), F32), V((max(n_sp - 1, 1), 8, mod_cols), F32),
        V((n_tp, 8, mod_cols), F32),
        V((rows, dk), BF16), V((rows, dk), BF16), V((rows, dv), BF16), V((rows, dv), BF16),
        V((rows, dk), F32), V((rows, dk), F32), V((rows, dv), F32), V((rows, dv), BF16),
        V((n_ctx, dk), BF16), V((n_ctx, dv), BF16), V((dv, dk), F32), V((dv, dk), F32),
    ]
    scratch += [V((dv, dk), BF16)] * 8
    scratch += [V((8, dk), F32)] * 4
    scratch += [
        V((n_tp,  n_dp, rows_own, w_out.shape[1]), BF16),
        V((n_tp - 1, n_dp, rows_own, w_out.shape[1]), BF16),
        D((8,)), D((n_dp - 1, 5)), D((n_dp - 1, 5)), D((n_tp - 1, 2)), D((n_tp - 1, 2)),
        D((n_sp - 1,)), D((n_sp - 1,)), D((n_tp - 1,)), D((n_tp - 1,)),
        D((4, CH)), D((4, CH)), D((2,)), D((2,)),
        D((n_tp - 1, n_dp)), D((n_tp - 1, n_dp)), D((1,)),
    ]
    out = pl.pallas_call(
        functools.partial(kernel, n_sp, n_tp, n_dp),
        out_shape=jax.ShapeDtypeStruct((1, rows_own, width), BF16),
        in_specs=[vm, vm, vm, vm, hbm, hbm, hbm, hbm, hbm, hbm, hbm, vm, vm, vm, hbm],
        out_specs=vm,
        scratch_shapes=scratch,
        compiler_params=pltpu.CompilerParams(
            collective_id=0, has_side_effects=True, vmem_limit_bytes=60 * 1024 * 1024
        ),
    )(
        latents, cond, vectors, context, w_shift, w_scale, w_gate, w_query, w_key, w_value,
        w_outgate, w_down.T, decay_up, decay_bias, w_out,
    )
    return out


def solution(mesh):
    return jax.shard_map(
        body,
        mesh=mesh,
        in_specs=(
            P("dp", ("sp", "tp"), None),
            P("dp", "sp"),
            P("sp"),
            P("dp", "sp", None),
            P("sp", "tp"),
            P("sp", "tp"),
            P("sp", "tp"),
            P(),
            P(),
            P("dp", "tp"),
            P("dp", "tp"),
            P("dp", "tp"),
            P("dp", "tp"),
            P(),
            P(None, None, "tp"),
            P(None, "tp"),
            P("tp"),
            P("tp", "dp"),
        ),
        out_specs=P("dp", ("sp", "tp"), None),
        check_vma=False,
    )
```

```python
import functools

import jax
import jax.numpy as jnp
from jax import lax
from jax.experimental import pallas as pl
from jax.experimental.pallas import tpu as pltpu
from jax.sharding import PartitionSpec as P

RANK = 16
EPS = 1e-06
TAU = 16.0
SUB = 64
CH = 8
MESH = pl.DeviceIdType.MESH
F32 = jnp.float32
BF16 = jnp.bfloat16


def dot(a, b, dims=((1,), (0,))):
    return lax.dot_general(a, b, (dims, ((), ())), preferred_element_type=F32)


def silu(v):
    return v / (1.0 + jnp.exp(-v))


def log_sigmoid(v):
    return jnp.minimum(v, 0.0) - jnp.log1p(jnp.exp(-jnp.abs(v)))


def tri_sum(tri, g):
    high = g.astype(BF16)
    low = (g - high.astype(F32)).astype(BF16)
    return dot(tri, high) + dot(tri, low)


def triangle(n, upper):
    row = lax.broadcasted_iota(jnp.int32, (n, n), 0)
    col = lax.broadcasted_iota(jnp.int32, (n, n), 1)
    keep = (col >= row) if upper else (col <= row)
    return jnp.where(keep, 1.0, 0.0).astype(BF16)


def kernel(
    n_sp, n_tp, n_dp,
    lat3, cond_ref, vec_ref, ctx3, wsh_hbm, wsc_hbm, wga_hbm,
    wq_hbm, wk_hbm, wv_hbm, wg_hbm, wdown_ref, up_ref, bias_ref, wout_hbm,
    out3,
    wsh, wsc, wga, wq, wk, wv, wg, wout,
    lat_all, rows_lat, rows_ctx, part, mod_sp, mod_full,
    qb, kb, vb, gb, cum_f, cum_b, intra, heads,
    kc, vc, st_a, st_b,
    ry, rz, rf, rb, sy, sz, sf, sb, ra_f, ra_b, sa_f, sa_b,
    rs_send, rs_recv,
    lc_sem, wsend, wrecv, lsend, lrecv, m1send, m1recv, m2send, m2recv,
    csend, crecv, asend, arecv, osend, orecv, own_sem,
):
    sp, tp, dp = lax.axis_index("sp"), lax.axis_index("tp"), lax.axis_index("dp")
    half = n_tp // 2
    ty, tx = tp // 2, tp % 2

    def to(k):
        return ((ty + k // 2) % half) * 2 + (tx + k % 2) % 2

    def source(k):
        return ((ty + half - k // 2) % half) * 2 + (tx + k % 2) % 2

    lat_ref, ctx_ref, out_ref = lat3.at[0], ctx3.at[0], out3.at[0]
    rows_own, width = lat_ref.shape
    n_cond, n_head = cond_ref.shape[1], vb.shape[1]
    gpre_ref = vec_ref.at[:, pl.ds(0, width)]
    gpost_ref = vec_ref.at[:, pl.ds(width, width)]
    cctx_ref = vec_ref.at[:, pl.ds(2 * width, n_cond)]
    hgain_ref = vec_ref.at[:, pl.ds(2 * width + n_cond, n_head)]
    rows = rows_own * n_tp
    cb = part.shape[1]

    def remote(src, dst, s, r, dev):
        return pltpu.make_async_remote_copy(
            src_ref=src, dst_ref=dst, send_sem=s, recv_sem=r, device_id=dev, device_id_type=MESH
        )

    mod_copies = []
    for i, (a, b) in enumerate(((wsh_hbm, wsh), (wsc_hbm, wsc), (wga_hbm, wga))):
        c = pltpu.make_async_copy(a, b, lc_sem.at[i])
        c.start()
        mod_copies.append(c)
    own = pltpu.make_async_copy(lat_ref, lat_all.at[tp], own_sem.at[0])
    own.start()

    barrier = pltpu.get_barrier_semaphore()
    for k in range(1, n_tp):
        pl.semaphore_signal(barrier, inc=1, device_id={"tp": to(k)}, device_id_type=MESH)
    for k in range(1, n_sp):
        pl.semaphore_signal(
            barrier, inc=1, device_id={"sp": (sp + k) % n_sp}, device_id_type=MESH
        )
    for k in range(1, n_dp):
        pl.semaphore_signal(
            barrier, inc=1, device_id={"dp": (dp + k) % n_dp}, device_id_type=MESH
        )
    pl.semaphore_wait(barrier, n_tp + n_sp + n_dp - 3)

    hr = rows_own // 2
    lat_copies = {}

    def send_lat(k, h):
        c = remote(
            lat_ref.at[pl.ds(h * hr, hr)], lat_all.at[tp, pl.ds(h * hr, hr)],
            lsend.at[k - 1, h], lrecv.at[k - 1, h], {"tp": to(k)},
        )
        c.start()
        lat_copies[k, h] = c

    for k in range(1, n_tp - 1):
        send_lat(k, 0)

    weight_pairs = ((wk_hbm, wk), (wv_hbm, wv), (wq_hbm, wq), (wg_hbm, wg), (wout_hbm, wout))
    w_copies = []
    for i, (a, b) in enumerate(weight_pairs):
        c = pltpu.make_async_copy(a, b.at[dp], lc_sem.at[3 + i])
        c.start()
        group = [c]
        for k in range(1, n_dp):
            c = remote(a, b.at[dp], wsend.at[k - 1, i], wrecv.at[k - 1, i],
                       {"dp": (dp + k) % n_dp})
            c.start()
            group.append(c)
        w_copies.append(group)

    def weights_ready(i):
        w_copies[i][0].wait()
        for c in w_copies[i][1:]:
            c.wait_recv()

    shape = (16, cond_ref.shape[1])
    first = lax.broadcasted_iota(jnp.int32, shape, 0) == 0
    act = jnp.where(
        first,
        jnp.broadcast_to(silu(cond_ref[...].astype(F32)), shape),
        jnp.broadcast_to(silu(cctx_ref[...].astype(F32)), shape),
    ).astype(BF16)
    for c in mod_copies:
        c.wait()
    d_sh, d_sc, d_ga = dot(act, wsh[...]), dot(act, wsc[...]), dot(act, wga[...])
    part[...] = jnp.zeros_like(part)
    part[0:1] = d_sh[0:1]
    part[1:2] = d_sc[0:1]
    part[2:3] = d_ga[0:1]
    part[3:4] = d_sh[1:2]
    part[4:5] = d_sc[1:2]
    m1 = []
    for k in range(1, n_sp):
        c = remote(part, mod_sp.at[k - 1], m1send.at[k - 1], m1recv.at[k - 1],
                   {"sp": (sp + k) % n_sp})
        c.start()
        m1.append(c)
    total = part[...]
    for k, c in enumerate(m1):
        c.wait_recv()
        total = total + mod_sp[k]
    mod_full[tp] = total
    m2 = []
    for k in range(1, n_tp):
        c = remote(mod_full.at[tp], mod_full.at[tp], m2send.at[k - 1], m2recv.at[k - 1],
                   {"tp": to(k)})
        c.start()
        m2.append(c)
    for k in (n_tp - 1,):
        send_lat(k, 0)
        send_lat(k, 1)
    for k in range(1, n_tp - 1):
        send_lat(k, 1)
    for c in m2:
        c.wait_recv()

    def modulate(load, store, count, at):
        def step(r, carry):
            x = load(r * 16).astype(F32)
            inv = lax.rsqrt(jnp.mean(x * x, axis=-1, keepdims=True) + EPS)
            pieces = []
            for c in range(n_tp):
                gain = gpre_ref[:, c * cb : (c + 1) * cb].astype(F32)
                y = x[:, c * cb : (c + 1) * cb] * inv * gain
                y = y * (1.0 + mod_full[c, at + 1 : at + 2]) + mod_full[c, at : at + 1]
                pieces.append(y.astype(BF16))
            store(r * 16, jnp.concatenate(pieces, axis=1))
            return carry

        lax.fori_loop(0, count // 16, step, 0)

    def project(src, w):
        depth = w.shape[1]
        acc = dot(src[:, 0:depth], w[0])
        for d in range(1, n_dp):
            acc = acc + dot(src[:, d * depth : (d + 1) * depth], w[d])
        return acc.astype(BF16)

    def decays(src):
        low = dot(src[...], wdown_ref[...], ((1,), (1,))).astype(BF16)
        zero = jnp.zeros_like(up_ref[0])
        both = jnp.concatenate(
            [
                jnp.concatenate([up_ref[0], zero], axis=1),
                jnp.concatenate([zero, up_ref[1]], axis=1),
            ],
            axis=0,
        )
        bias = jnp.concatenate([bias_ref[0:1], bias_ref[1:2]], axis=1)
        return log_sigmoid(dot(low, both) + bias) * (1.0 / TAU)

    n_ctx = ctx_ref.shape[0]

    def store_ctx(r, val):
        rows_ctx[pl.ds(pl.multiple_of(r, 16), 16)] = val

    modulate(lambda r: ctx_ref[pl.ds(pl.multiple_of(r, 16), 16)], store_ctx, n_ctx, 3)
    weights_ready(0)
    weights_ready(1)
    dk = kb.shape[1]
    dv = vb.shape[1]
    kc[...] = project(rows_ctx, wk)
    vc[...] = project(rows_ctx, wv)
    g_ctx = decays(rows_ctx)
    cum = tri_sum(triangle(n_ctx, False), g_ctx)
    keys = kc[...].astype(F32)
    last = cum[n_ctx - 1 : n_ctx]
    key_f = (keys * jnp.exp(last[:, :dk] - cum[:, :dk])).astype(BF16)
    key_b = (keys * jnp.exp(cum[:, dk:] - g_ctx[:, dk:])).astype(BF16)
    st_a[...] = dot(vc[...], key_f, ((0,), (0,)))
    st_b[...] = dot(vc[...], key_b, ((0,), (0,)))
    tot_f = last[:, :dk]
    tot_b = last[:, dk:]

    up = {"sp": jnp.minimum(sp + 1, n_sp - 1)}
    down = {"sp": jnp.maximum(sp - 1, 0)}
    has_up = sp < n_sp - 1
    has_down = sp > 0
    cw = dv // CH

    def chunk(i):
        return pl.ds(i * cw, cw)

    def y_copy(i):
        return remote(sy.at[chunk(i)], ry.at[chunk(i)], csend.at[0, i], crecv.at[0, i], down)

    def z_copy(i):
        return remote(sz.at[chunk(i)], rz.at[chunk(i)], csend.at[1, i], crecv.at[1, i], up)

    def f_copy(i):
        return remote(sf.at[chunk(i)], rf.at[chunk(i)], csend.at[2, i], crecv.at[2, i], up)

    def b_copy(i):
        return remote(sb.at[chunk(i)], rb.at[chunk(i)], csend.at[3, i], crecv.at[3, i], down)

    a_f = remote(sa_f, ra_f, asend.at[0], arecv.at[0], down)
    a_b = remote(sa_b, ra_b, asend.at[1], arecv.at[1], up)

    @pl.when(jnp.logical_not(has_up))
    def _():
        ra_f[...] = jnp.zeros_like(ra_f)
        ry[...] = jnp.zeros_like(ry)

    @pl.when(jnp.logical_not(has_down))
    def _():
        ra_b[...] = jnp.zeros_like(ra_b)
        rz[...] = jnp.zeros_like(rz)

    def a_down():
        @pl.when(has_up)
        def _():
            a_f.wait_recv()

        sa_f[...] = ra_f[...] + tot_f

        @pl.when(has_down)
        def _():
            a_f.start()

    def a_up():
        @pl.when(has_down)
        def _():
            a_b.wait_recv()

        sa_b[...] = ra_b[...] + tot_b

        @pl.when(has_up)
        def _():
            a_b.start()

    lower = 2 * sp < n_sp
    upper = jnp.logical_not(lower)
    pl.when(lower)(a_up)
    pl.when(upper)(a_down)
    pl.when(lower)(a_down)
    pl.when(upper)(a_up)

    scale_f = jnp.exp(ra_f[0:1])
    scale_b = jnp.exp(ra_b[0:1])
    def modulate_block(blk):
        def store(r, val):
            at = pl.multiple_of(blk * rows_own + r, 16)
            rows_lat[pl.ds(at, 16)] = val

        modulate(
            lambda r: lat_all[blk, pl.ds(pl.multiple_of(r, 16), 16)], store, rows_own, 0
        )

    def y_pass():
        for i in range(CH):
            c = slice(i * cw, (i + 1) * cw)

            @pl.when(has_up)
            def _():
                y_copy(i).wait_recv()

            sy[c] = (ry[c].astype(F32) + st_a[c] * scale_f).astype(BF16)

            @pl.when(has_down)
            def _():
                y_copy(i).start()

    def z_pass():
        for i in range(CH):
            c = slice(i * cw, (i + 1) * cw)

            @pl.when(has_down)
            def _():
                z_copy(i).wait_recv()

            sz[c] = (rz[c].astype(F32) + st_b[c] * scale_b).astype(BF16)

            @pl.when(has_up)
            def _():
                z_copy(i).start()

    pl.when(lower)(z_pass)
    pl.when(upper)(y_pass)
    own.wait()
    modulate_block(tp)
    pl.when(lower)(y_pass)
    pl.when(upper)(z_pass)

    @pl.when(jnp.logical_not(has_down))
    def _():
        rf[...] = sy[...]

    @pl.when(jnp.logical_not(has_up))
    def _():
        rb[...] = sz[...]

    for k in range(1, n_tp):
        lat_copies[k, 0].wait_recv()
        lat_copies[k, 1].wait_recv()
        modulate_block(source(k))

    kb[...] = project(rows_lat, wk)
    vb[...] = project(rows_lat, wv)
    g_lat = decays(rows_lat)
    cum_f[...] = tri_sum(triangle(rows, False), g_lat[:, :dk])
    cum_b[...] = tri_sum(triangle(rows, True), g_lat[:, dk:])
    keys = kb[...].astype(F32)
    end_f = cum_f[rows - 1 : rows]
    end_b = cum_b[0:1]
    key_f = (keys * jnp.exp(end_f - cum_f[...])).astype(BF16)
    key_b = (keys * jnp.exp(end_b - cum_b[...])).astype(BF16)
    st_a[...] = dot(vb[...], key_f, ((0,), (0,)))
    st_b[...] = dot(vb[...], key_b, ((0,), (0,)))
    step_f = jnp.exp(end_f)
    step_b = jnp.exp(end_b)

    def f_pass():
        for i in range(CH):
            c = slice(i * cw, (i + 1) * cw)

            @pl.when(has_down)
            def _():
                f_copy(i).wait_recv()

            @pl.when(has_up)
            def _():
                sf[c] = (rf[c].astype(F32) * step_f + st_a[c]).astype(BF16)
                f_copy(i).start()

    def b_pass():
        for i in range(CH):
            c = slice(i * cw, (i + 1) * cw)

            @pl.when(has_up)
            def _():
                b_copy(i).wait_recv()

            @pl.when(has_down)
            def _():
                sb[c] = (rb[c].astype(F32) * step_b + st_b[c]).astype(BF16)
                b_copy(i).start()

    pl.when(lower)(f_pass)
    pl.when(upper)(b_pass)

    weights_ready(2)
    weights_ready(3)
    qb[...] = project(rows_lat, wq)
    gb[...] = project(rows_lat, wg)

    scale = dk ** -0.5
    n_sub = rows // SUB

    def block_scores(i):
        lo, hi, mid = i * SUB, (i + 1) * SUB, i * SUB + SUB // 2
        q = qb[lo:hi].astype(F32) * scale
        r_f = cum_f[mid : mid + 1]
        s_f = dot(
            (q * jnp.exp(cum_f[lo:hi] - r_f)).astype(BF16),
            (kb[0:hi].astype(F32) * jnp.exp(r_f - cum_f[0:hi])).astype(BF16),
            ((1,), (1,)),
        )
        t = lax.broadcasted_iota(jnp.int32, (SUB, hi), 0) + lo
        s = lax.broadcasted_iota(jnp.int32, (SUB, hi), 1)
        s_f = jnp.where(s <= t, s_f, 0.0)
        r_b = cum_b[mid : mid + 1]
        s_b = dot(
            (q * jnp.exp(cum_b[lo:hi] - r_b)).astype(BF16),
            (kb[lo:rows].astype(F32) * jnp.exp(r_b - cum_b[lo:rows])).astype(BF16),
            ((1,), (1,)),
        )
        t = lax.broadcasted_iota(jnp.int32, (SUB, rows - lo), 0)
        s = lax.broadcasted_iota(jnp.int32, (SUB, rows - lo), 1)
        s_b = jnp.where(s >= t, s_b, 0.0)
        intra[lo:hi] = dot(s_f.astype(BF16), vb[0:hi]) + dot(s_b.astype(BF16), vb[lo:rows])

    for i in range(n_sub):
        block_scores(i)
    pl.when(lower)(b_pass)
    pl.when(upper)(f_pass)

    q = qb[...].astype(F32) * scale
    q_f = (q * jnp.exp(cum_f[...])).astype(BF16)
    q_b = (q * jnp.exp(cum_b[...])).astype(BF16)
    mixed = intra[...] + dot(q_f, rf[...], ((1,), (1,))) + dot(q_b, rb[...], ((1,), (1,)))
    inv = lax.rsqrt(jnp.mean(mixed * mixed, axis=-1, keepdims=True) + EPS)
    gated = mixed * inv * hgain_ref[...].astype(F32) * silu(gb[...].astype(F32))
    heads[...] = gated.astype(BF16)

    weights_ready(4)
    out_copies = []
    wc = wout.shape[2]
    for k in list(range(n_tp - 1, 0, -1)) + [0]:
        h = heads[pl.ds(pl.multiple_of(to(k) * rows_own, rows_own), rows_own)]
        for d in range(n_dp):
            rs_send[k, d] = dot(h, wout[d]).astype(BF16)
            if k:
                c = remote(rs_send.at[k, d], rs_recv.at[k - 1, d], osend.at[k - 1, d],
                           orecv.at[k - 1, d], {"tp": to(k)})
                c.start()
                out_copies.append(c)
    for c in out_copies:
        c.wait_recv()

    def finish(r, carry):
        at = pl.ds(pl.multiple_of(r * 16, 16), 16)
        proj = []
        for d in range(n_dp):
            v = rs_send[0, d, at].astype(F32)
            for k in range(1, n_tp):
                v = v + rs_recv[k - 1, d, at].astype(F32)
            proj.append(v)
        v = jnp.concatenate(proj, axis=1)
        inv = lax.rsqrt(jnp.mean(v * v, axis=-1, keepdims=True) + EPS)
        x = lat_ref[at].astype(F32)
        for c in range(n_tp):
            cols = slice(c * cb, (c + 1) * cb)
            y = v[:, cols] * inv * gpost_ref[:, cols].astype(F32)
            out_ref[at, cols] = (x[:, cols] + mod_full[c, 2:3] * y).astype(BF16)
        return carry

    lax.fori_loop(0, rows_own // 16, finish, 0)

    for c in out_copies + m1 + m2 + list(lat_copies.values()):
        c.wait_send()
    for group in w_copies:
        for c in group[1:]:
            c.wait_send()

    @pl.when(has_down)
    def _():
        a_f.wait_send()
        for i in range(CH):
            y_copy(i).wait_send()
            b_copy(i).wait_send()

    @pl.when(has_up)
    def _():
        a_b.wait_send()
        for i in range(CH):
            z_copy(i).wait_send()
            f_copy(i).wait_send()


def body(
    latents, cond, cond_ctx, context, w_shift, w_scale, w_gate, gain_pre, gain_post,
    w_query, w_key, w_value, w_outgate, w_down, decay_up, decay_bias, head_gain, w_out,
):
    n_sp, n_tp, n_dp = lax.axis_size("sp"), lax.axis_size("tp"), lax.axis_size("dp")
    width = gain_pre.shape[0]
    rows_own = latents.shape[1]
    rows = rows_own * n_tp
    n_ctx = context.shape[1]
    dk, dv = w_key.shape[1], w_value.shape[1]
    depth = w_key.shape[0]
    vectors = lax.optimization_barrier(
        jnp.concatenate([gain_pre, gain_post, cond_ctx, head_gain])
    )[None]
    mod_in, mod_cols = w_shift.shape
    vm = pl.BlockSpec(memory_space=pltpu.VMEM)
    hbm = pl.BlockSpec(memory_space=pl.ANY)
    V, D = pltpu.VMEM, pltpu.SemaphoreType.DMA
    scratch = [
        V((mod_in, mod_cols), BF16), V((mod_in, mod_cols), BF16), V((mod_in, mod_cols), BF16),
        V((n_dp, depth, dk), BF16), V((n_dp, depth, dk), BF16),
        V((n_dp, depth, dv), BF16), V((n_dp, depth, dv), BF16),
        V((n_dp,) + w_out.shape, BF16),
        V((n_tp, rows_own, width), BF16), V((rows, width), BF16), V((n_ctx, width), BF16),
        V((8, mod_cols), F32), V((max(n_sp - 1, 1), 8, mod_cols), F32),
        V((n_tp, 8, mod_cols), F32),
        V((rows, dk), BF16), V((rows, dk), BF16), V((rows, dv), BF16), V((rows, dv), BF16),
        V((rows, dk), F32), V((rows, dk), F32), V((rows, dv), F32), V((rows, dv), BF16),
        V((n_ctx, dk), BF16), V((n_ctx, dv), BF16), V((dv, dk), F32), V((dv, dk), F32),
    ]
    scratch += [V((dv, dk), BF16)] * 8
    scratch += [V((8, dk), F32)] * 4
    scratch += [
        V((n_tp,  n_dp, rows_own, w_out.shape[1]), BF16),
        V((n_tp - 1, n_dp, rows_own, w_out.shape[1]), BF16),
        D((8,)), D((n_dp - 1, 5)), D((n_dp - 1, 5)), D((n_tp - 1, 2)), D((n_tp - 1, 2)),
        D((n_sp - 1,)), D((n_sp - 1,)), D((n_tp - 1,)), D((n_tp - 1,)),
        D((4, CH)), D((4, CH)), D((2,)), D((2,)),
        D((n_tp - 1, n_dp)), D((n_tp - 1, n_dp)), D((1,)),
    ]
    out = pl.pallas_call(
        functools.partial(kernel, n_sp, n_tp, n_dp),
        out_shape=jax.ShapeDtypeStruct((1, rows_own, width), BF16),
        in_specs=[vm, vm, vm, vm, hbm, hbm, hbm, hbm, hbm, hbm, hbm, vm, vm, vm, hbm],
        out_specs=vm,
        scratch_shapes=scratch,
        compiler_params=pltpu.CompilerParams(
            collective_id=0, has_side_effects=True, vmem_limit_bytes=60 * 1024 * 1024
        ),
    )(
        latents, cond, vectors, context, w_shift, w_scale, w_gate, w_query, w_key, w_value,
        w_outgate, w_down.T, decay_up, decay_bias, w_out,
    )
    return out


def solution(mesh):
    return jax.shard_map(
        body,
        mesh=mesh,
        in_specs=(
            P("dp", ("sp", "tp"), None),
            P("dp", "sp"),
            P("sp"),
            P("dp", "sp", None),
            P("sp", "tp"),
            P("sp", "tp"),
            P("sp", "tp"),
            P(),
            P(),
            P("dp", "tp"),
            P("dp", "tp"),
            P("dp", "tp"),
            P("dp", "tp"),
            P(),
            P(None, None, "tp"),
            P(None, "tp"),
            P("tp"),
            P("tp", "dp"),
        ),
        out_specs=P("dp", ("sp", "tp"), None),
        check_vma=False,
    )
```
